32 devices in a mesh: sp: 8 (over z, x), tp: 4 (over y, core).
Axes of the slice: x: 2, y: 2, z: 4, core: 2. Of those that a mesh axis runs over, the one named last changes fastest.
Arguments:
- queries: bfloat16 [5120, 2048], P('sp', 'tp'), may hold values from -164 to 164
- keys: bfloat16 [5120, 512], P('sp', 'tp'), may hold values from -6 to 6
- values: bfloat16 [5120, 512], P('sp', 'tp'), may hold values from -6 to 6
- sink: float32 [32], P('tp'), may hold values from 4 to 8
- stream: bfloat16 [5120, 2048], P(('sp', 'tp')), may hold values from -6 to 6
- out_weight: bfloat16 [2048, 2048], P('tp'), may hold values from -0.5390625 to 0.5390625
- norm_gain: float32 [2048], replicated, may hold values from 0.1 to 1.9
- gate_weight: bfloat16 [2048, 5632], P('sp', 'tp'), may hold values from -0.125 to 0.125
- up_weight: bfloat16 [2048, 5632], P('sp', 'tp'), may hold values from -0.125 to 0.125
- down_weight: bfloat16 [5632, 2048], P('tp', 'sp'), may hold values from -0.23925781 to 0.23925781
Outputs:
- result: bfloat16 [5120, 2048], P(('sp', 'tp'))
The draws below stay inside these ranges and needn't reach their ends.
All inputs are finite; a program needn't handle non-finite values.
Results may differ from the reference program's by a relative error of at most 0.019.
Values may be sent and summed in bfloat16 or wider, within the bound.
A program may use at most 128 MiB of HBM per device.

```python
import jax
import jax.numpy as jnp
from jax import lax

D = 2048
HEADS = 32
KV_HEADS = 8
HEAD = 64
FF = 5632
WINDOW = 128
TOK_DEV = 640
TOKENS = 5120


def draw_queries(key, part):
    shape = (TOKENS, HEADS * HEAD)
    return jnp.clip(2.0 * jax.random.normal(key, shape, jnp.float32), -12.0, 12.0).astype(jnp.bfloat16)


def block_scale(key, shape, cuts, least, largest):
    def one(axis_at, shards_of):
        steps = jax.random.uniform(jax.random.fold_in(jax.random.fold_in(key, 6), axis_at), (shards_of,), jnp.float32, least / len(cuts), largest / len(cuts))
        return jnp.repeat(jnp.exp(steps), shape[axis_at] // shards_of).reshape((-1,) + (1,) * (len(shape) - axis_at - 1))

    gain = one(*cuts[0])
    for cut in cuts[1:]:
        gain = gain * one(*cut)
    return gain


def normal_values(own_key, extent, width, bound, cuts=(), held_as=jnp.bfloat16):
    level = block_scale(own_key, extent, cuts, -0.22, 0.18) if cuts else 1.0
    array = jax.random.normal(own_key, extent, jnp.float32) * width * level
    return jnp.minimum(jnp.maximum(array, -bound), bound).astype(held_as)


def setup_inputs(seed: int = 0) -> dict:
    key_list = jax.random.split(jax.random.key(seed), 11)
    return {
        "queries": draw_queries(jax.random.fold_in(key_list[10], 71), 0),
        "keys": normal_values(key_list[1], (TOKENS, KV_HEADS * HEAD), 1.0, 6.0, ((0, 8), (1, 4))),
        "values": normal_values(key_list[2], (TOKENS, KV_HEADS * HEAD), 1.0, 6.0, ((0, 8), (1, 4))),
        "sink": jnp.clip(4.0 + 4.0 * jax.random.uniform(key_list[3], (HEADS,), jnp.float32) ** block_scale(key_list[3], (HEADS,), ((0, 4),), -0.2, 0.2), 4.0, 8.0),
        "stream": normal_values(key_list[4], (TOKENS, D), 1.0, 6.0, ((0, 32),)),
        "out_weight": normal_values(key_list[5], (HEADS * HEAD, D), 0.09, 0.5390625, ((0, 4),)),
        "norm_gain": jnp.clip(1.0 + 0.18 * jax.random.normal(key_list[6], (D,), jnp.float32), 0.1, 1.9),
        "gate_weight": normal_values(key_list[7], (D, FF), D ** -0.5, 0.125, ((0, 8), (1, 4))),
        "up_weight": normal_values(key_list[8], (D, FF), D ** -0.5, 0.125, ((0, 8), (1, 4))),
        "down_weight": normal_values(key_list[9], (FF, D), 0.04, 0.23925781, ((0, 4), (1, 8))),
    }


def rotary(block, start):
    length = block.shape[0]
    middle = HEAD // 2
    inverse = 1.0 / 10000.0 ** (jnp.arange(0, HEAD, 2, dtype=jnp.float32) / HEAD)
    places = (start + jnp.arange(length, dtype=jnp.int32)).astype(jnp.float32)
    angles = places[:, None, None] * inverse[None, None, :]
    cosine_table = jnp.cos(angles)
    sine_table = jnp.sin(angles)
    pieces = block.astype(jnp.float32).reshape(length, -1, HEAD)
    leading = pieces[..., :middle]
    trailing = pieces[..., middle:]
    turned = jnp.concatenate([leading * cosine_table - trailing * sine_table, trailing * cosine_table + leading * sine_table], -1)
    return turned.reshape(length, -1).astype(jnp.bfloat16)

def reference(queries, keys, values, sink, stream, out_weight, norm_gain, gate_weight, up_weight, down_weight):
    length = queries.shape[0]
    blocks = length // WINDOW
    group = HEADS // KV_HEADS
    kv_width = KV_HEADS * HEAD
    turned_q = rotary(queries, 0)
    turned_k = rotary(keys, 0)
    paired = jnp.concatenate([turned_k, values], 1)
    padded = jnp.pad(paired, ((WINDOW, WINDOW), (0, 0)))
    framed = padded.reshape(blocks + 2, WINDOW, 2 * kv_width)
    banded = jnp.concatenate([framed[:-2], framed[1:-1], framed[2:]], axis=1)
    key_band = jnp.moveaxis(banded[..., :kv_width].reshape(blocks, 3 * WINDOW, KV_HEADS, HEAD), 2, 0)
    value_band = jnp.moveaxis(banded[..., kv_width:].reshape(blocks, 3 * WINDOW, KV_HEADS, HEAD), 2, 0)
    query_blocks = jnp.moveaxis(turned_q.reshape(blocks, WINDOW, KV_HEADS, group, HEAD), 2, 0)
    sink_grid = sink.reshape(KV_HEADS, group)
    query_place = jnp.arange(blocks)[:, None, None] * WINDOW + jnp.arange(WINDOW)[None, :, None]
    key_place = jnp.arange(blocks)[:, None, None] * WINDOW - WINDOW + jnp.arange(3 * WINDOW)[None, None, :]
    valid = (jnp.abs(key_place - query_place) <= WINDOW) & (key_place >= 0) & (key_place < length)

    def one_head(item):
        query_part, key_part, value_part, sink_part = item
        scores = jnp.einsum('nqgd,nsd->ngqs', query_part.astype(jnp.float32), key_part.astype(jnp.float32)) * HEAD ** (-0.5)
        scores = jnp.where(valid[:, None], scores, -jnp.inf)
        sink_here = sink_part[None, :, None]
        top = jnp.maximum(lax.optimization_barrier(jnp.max(scores, -1)), sink_here)
        raised = jnp.exp(scores - top[..., None])
        denom = lax.optimization_barrier(jnp.sum(raised, -1)) + jnp.exp(sink_here - top)
        weights = lax.optimization_barrier((raised / denom[..., None]).astype(jnp.bfloat16))
        output = jnp.einsum('ngqs,nsd->nqgd', weights.astype(jnp.float32), value_part.astype(jnp.float32))
        return output.astype(jnp.bfloat16)
    heads_out = lax.map(one_head, (query_blocks, key_band, value_band, sink_grid))
    attended = jnp.moveaxis(heads_out, 0, 2).reshape(length, HEADS * HEAD)
    mixed = (stream.astype(jnp.float32) + jnp.dot(attended, out_weight, preferred_element_type=jnp.float32)).astype(jnp.bfloat16)
    mixed_wide = mixed.astype(jnp.float32)
    scale = lax.rsqrt(lax.optimization_barrier(jnp.mean(mixed_wide * mixed_wide, -1, keepdims=True)) + 1e-06)
    normed = (mixed_wide * scale * norm_gain).astype(jnp.bfloat16)

    def feed_forward(rows):
        gate = jnp.dot(rows, gate_weight, preferred_element_type=jnp.float32)
        upward = jnp.dot(rows, up_weight, preferred_element_type=jnp.float32)
        hidden = (jax.nn.silu(gate) * upward).astype(jnp.bfloat16)
        return jnp.dot(hidden, down_weight, preferred_element_type=jnp.float32)
    lowered = lax.map(feed_forward, normed.reshape(-1, TOK_DEV, D)).reshape(length, D)
    return (mixed_wide + 0.5 * lowered).astype(jnp.bfloat16)
```

```python
import jax
import jax.numpy as jnp
from jax import lax
from jax.sharding import PartitionSpec as P

HEAD = 64
WINDOW = 128
BF = jnp.bfloat16
F32 = jnp.float32


def padded_2(cells, sides, width):
    for axis, dim in sides:
        count = lax.axis_size(axis)
        ends = count - 1
        head = lax.slice_in_dim(cells, 0, width, axis=dim)
        tail = lax.slice_in_dim(cells, cells.shape[dim] - width, cells.shape[dim], axis=dim)
        cells = jnp.concatenate(
            [
                lax.ppermute(tail, axis, [(i, (i + 1) % count) for i in range(ends)]),
                cells,
                lax.ppermute(head, axis, [((i + 1) % count, i) for i in range(ends)]),
            ],
            axis=dim,
        )
    return cells


def rotary(block, start):
    length = block.shape[0]
    middle = HEAD // 2
    inverse = 1.0 / 10000.0 ** (jnp.arange(0, HEAD, 2, dtype=jnp.float32) / HEAD)
    places = (start + jnp.arange(length, dtype=jnp.int32)).astype(jnp.float32)
    angles = places[:, None, None] * inverse[None, None, :]
    cosine_table = jnp.cos(angles)
    sine_table = jnp.sin(angles)
    pieces = block.astype(jnp.float32).reshape(length, -1, HEAD)
    leading = pieces[..., :middle]
    trailing = pieces[..., middle:]
    turned = jnp.concatenate(
        [
            leading * cosine_table - trailing * sine_table,
            trailing * cosine_table + leading * sine_table,
        ],
        -1,
    )
    return turned.reshape(length, -1).astype(jnp.bfloat16)


def window_attend(queries, keys, values, sink):
    rows_here = queries.shape[0]
    start = lax.axis_index("sp") * rows_here
    length = lax.axis_size("sp") * rows_here
    blocks = rows_here // WINDOW
    kv_width = keys.shape[1]
    kv_count = kv_width // HEAD
    head_count = queries.shape[1] // HEAD
    group = head_count // kv_count
    turned_q = rotary(queries, start)
    wide = padded_2(jnp.concatenate([keys, values], 1), (("sp", 0),), WINDOW)
    turned_k = rotary(wide[:, :kv_width], start - WINDOW)
    padded = jnp.concatenate([turned_k, wide[:, kv_width:]], 1)
    framed = padded.reshape(blocks + 2, WINDOW, 2 * kv_width)
    banded = jnp.concatenate([framed[:-2], framed[1:-1], framed[2:]], axis=1)
    key_band = banded[..., :kv_width].reshape(blocks, 3 * WINDOW, kv_count, HEAD)
    value_band = banded[..., kv_width:].reshape(blocks, 3 * WINDOW, kv_count, HEAD)
    query_blocks = turned_q.reshape(blocks, WINDOW, kv_count, group, HEAD)
    scores = jnp.einsum(
        "nqkgd,nskd->nkgqs", query_blocks, key_band, preferred_element_type=jnp.float32
    ) * HEAD ** (-0.5)
    query_place = (
        start + jnp.arange(blocks)[:, None, None] * WINDOW + jnp.arange(WINDOW)[None, :, None]
    )
    key_place = (
        start
        + jnp.arange(blocks)[:, None, None] * WINDOW
        - WINDOW
        + jnp.arange(3 * WINDOW)[None, None, :]
    )
    valid = (jnp.abs(key_place - query_place) <= WINDOW) & (key_place >= 0) & (key_place < length)
    scores = jnp.where(valid[:, None, None], scores, -jnp.inf)
    sink_grid = sink.reshape(kv_count, group)[None, :, :, None]
    top = jnp.maximum(jnp.max(scores, -1), sink_grid)
    raised = jnp.exp(scores - top[..., None])
    denom = jnp.sum(raised, -1) + jnp.exp(sink_grid - top)
    weights = (raised / denom[..., None]).astype(jnp.bfloat16)
    output = jnp.einsum(
        "nkgqs,nskd->nqkgd", weights, value_band, preferred_element_type=jnp.float32
    )
    return output.astype(jnp.bfloat16).reshape(rows_here, head_count * HEAD)


def collect_weights(gate_weight, up_weight, down_weight):
    return (
        lax.all_gather(gate_weight, "sp", axis=0, tiled=True),
        lax.all_gather(up_weight, "sp", axis=0, tiled=True),
        lax.all_gather(down_weight, "sp", axis=1, tiled=True),
    )


def local(
    queries, keys, values, sink, stream, out_weight, norm_gain, gate_weight, up_weight, down_weight
):
    attended = window_attend(queries, keys, values, sink)
    gathered = collect_weights(gate_weight, up_weight, down_weight)
    gate_whole, up_whole, down_whole = gathered
    rows = attended
    projected = lax.psum_scatter(
        jnp.dot(rows, out_weight, preferred_element_type=jnp.float32),
        "tp",
        scatter_dimension=0,
        tiled=True,
    )
    mixed = (stream.astype(jnp.float32) + projected).astype(jnp.bfloat16)
    mixed_wide = mixed.astype(jnp.float32)
    scale = lax.rsqrt(jnp.mean(mixed_wide * mixed_wide, -1, keepdims=True) + 1e-06)
    normed = (mixed_wide * scale * norm_gain).astype(jnp.bfloat16)
    piece = lax.all_gather(normed, "tp", axis=0, tiled=True)
    gate = jnp.dot(piece, gate_whole, preferred_element_type=jnp.float32)
    upward = jnp.dot(piece, up_whole, preferred_element_type=jnp.float32)
    hidden = (jax.nn.silu(gate) * upward).astype(jnp.bfloat16)
    rows = hidden
    lowered = lax.psum_scatter(
        jnp.dot(rows, down_whole, preferred_element_type=jnp.float32).astype(jnp.bfloat16),
        "tp",
        scatter_dimension=0,
        tiled=True,
    ).astype(jnp.float32)
    return (mixed_wide + 0.5 * lowered).astype(jnp.bfloat16)


def swap(cells, axis, bit):
    count = lax.axis_size(axis)
    return lax.ppermute(cells, axis, [(i, i ^ bit) for i in range(count)])


def line_gather(piece, z, length):
    count = 2 * length
    up = [(i, i + 2) for i in range(count - 2)]
    down = [(i + 2, i) for i in range(count - 2)]
    rising, falling = [piece], [piece]
    for _ in range(length - 1):
        rising.append(lax.ppermute(rising[-1], "sp", up))
        falling.append(lax.ppermute(falling[-1], "sp", down))
    return [piece] + [
        jnp.where(z >= k, rising[k], falling[length - k]) for k in range(1, length)
    ]


def local_lines(
    queries, keys, values, sink, stream, out_weight, norm_gain, gate_weight, up_weight, down_weight
):
    length = lax.axis_size("sp") // 2
    s = lax.axis_index("sp")
    z, x = s // 2, s % 2
    t = lax.axis_index("tp")
    y, c = t // 2, t % 2
    depth, wide = gate_weight.shape
    half = wide // 2
    model = stream.shape[1]
    rows = stream.shape[0]

    low = jnp.concatenate([gate_weight[:, :half], up_weight[:, :half]], 1)
    high = jnp.concatenate([gate_weight[:, half:], up_weight[:, half:]], 1)
    first = x == 0
    gu_own = jnp.where(first, low, high)
    gu_other = swap(jnp.where(first, high, low), "sp", 1)
    d_own = jnp.where(first, down_weight[:half], down_weight[half:])
    d_other = swap(jnp.where(first, down_weight[half:], down_weight[:half]), "sp", 1)
    gu_own_slots = line_gather(gu_own, z, length)
    gu_other_slots = line_gather(gu_other, z, length)
    d_own_slots = line_gather(d_own, z, length)
    d_other_slots = line_gather(d_other, z, length)
    gu_whole = jnp.zeros((2 * length * depth, 2 * half), BF)
    for k in range(length):
        at = 2 * ((z - k) % length)
        gu_whole = lax.dynamic_update_slice_in_dim(
            gu_whole, gu_own_slots[k], (at + x) * depth, 0
        )
        gu_whole = lax.dynamic_update_slice_in_dim(
            gu_whole, gu_other_slots[k], (at + 1 - x) * depth, 0
        )

    attended = window_attend(queries, keys, values, sink)
    blocks = attended.reshape(2, 2, rows, attended.shape[1])
    blocks = jnp.where(y == 0, blocks, blocks[::-1])
    near = jnp.where(c == 0, blocks[:, 0], blocks[:, 1]).reshape(2 * rows, -1)
    far = jnp.where(c == 0, blocks[:, 1], blocks[:, 0]).reshape(2 * rows, -1)
    sent = jnp.dot(far, out_weight, preferred_element_type=F32).astype(BF)
    kept = jnp.dot(near, out_weight, preferred_element_type=F32)
    kept = kept + swap(sent, "tp", 1).astype(F32)
    projected = kept[:rows] + swap(kept[rows:].astype(BF), "tp", 2).astype(F32)
    mixed = (stream.astype(F32) + projected).astype(BF)
    mixed_wide = mixed.astype(F32)
    scale = lax.rsqrt(jnp.mean(mixed_wide * mixed_wide, -1, keepdims=True) + 1e-06)
    normed = (mixed_wide * scale * norm_gain).astype(BF)

    cut = model // 2
    a0, b0 = normed[:, :cut], normed[:, cut:]
    a_x = jnp.concatenate([a0, swap(a0, "sp", 1)], 0)
    b1 = swap(b0, "tp", 2)
    a_y = swap(a_x, "tp", 2)
    b_x = swap(jnp.concatenate([b0, b1], 0), "sp", 1)
    left = jnp.concatenate([a_x, a_y], 0)
    right = jnp.concatenate([b0, b_x[:rows], b1, b_x[rows:]], 0)
    piece_near = jnp.concatenate([left, right], 1)
    piece_far = swap(piece_near, "tp", 1)

    def hidden_of(piece):
        both = jnp.dot(piece, gu_whole, preferred_element_type=F32)
        return (jax.nn.silu(both[:, :half]) * both[:, half:]).astype(BF)

    hidden_near, hidden_far = hidden_of(piece_near), hidden_of(piece_far)
    lowered = jnp.zeros((rows, model), F32)
    for k in range(length):
        own, other = d_own_slots[k], d_other_slots[k]
        slot = jnp.concatenate(
            [jnp.where(first, own, other), jnp.where(first, other, own)], 1
        )
        width = slot.shape[1]
        sent = jnp.dot(hidden_far, slot, preferred_element_type=F32).astype(BF)
        kept = jnp.dot(hidden_near, slot, preferred_element_type=F32)
        kept = (kept + swap(sent, "tp", 1).astype(F32)).reshape(2, 2, rows, width)
        a, b = kept[..., : width // 2], kept[..., width // 2 :]
        a = a[:, 0] + swap(a[:, 1].astype(BF), "sp", 1).astype(F32)
        b = b[0] + swap(b[1].astype(BF), "tp", 2).astype(F32)
        a = a[0] + swap(a[1].astype(BF), "tp", 2).astype(F32)
        b = b[0] + swap(b[1].astype(BF), "sp", 1).astype(F32)
        lowered = lax.dynamic_update_slice_in_dim(
            lowered, jnp.concatenate([a, b], 1), ((z - k) % length) * width, 1
        )
    return (mixed_wide + 0.5 * lowered).astype(BF)


def solution(mesh):
    placed = (
        P("sp", "tp"),
        P("sp", "tp"),
        P("sp", "tp"),
        P("tp"),
        P(("sp", "tp"), None),
        P("tp", None),
        P(),
        P("sp", "tp"),
        P("sp", "tp"),
        P("tp", "sp"),
    )
    lines = mesh.shape["tp"] == 4 and mesh.shape["sp"] in (4, 8)
    return jax.shard_map(
        local_lines if lines else local, mesh=mesh, in_specs=placed, out_specs=P(("sp", "tp"), None), check_vma=False
    )
```

```python
import functools

import jax
import jax.numpy as jnp
from jax import lax
from jax.experimental import pallas as pl
from jax.experimental.pallas import tpu as pltpu
from jax.sharding import PartitionSpec as P

HEAD = 64
WINDOW = 128
LANES = 128
BF = jnp.bfloat16
F32 = jnp.float32
MESH = pl.DeviceIdType.MESH


def padded_2(cells, sides, width):
    for axis, dim in sides:
        count = lax.axis_size(axis)
        ends = count - 1
        head = lax.slice_in_dim(cells, 0, width, axis=dim)
        tail = lax.slice_in_dim(cells, cells.shape[dim] - width, cells.shape[dim], axis=dim)
        cells = jnp.concatenate(
            [
                lax.ppermute(tail, axis, [(i, (i + 1) % count) for i in range(ends)]),
                cells,
                lax.ppermute(head, axis, [((i + 1) % count, i) for i in range(ends)]),
            ],
            axis=dim,
        )
    return cells


def rotary(block, start):
    length = block.shape[0]
    middle = HEAD // 2
    inverse = 1.0 / 10000.0 ** (jnp.arange(0, HEAD, 2, dtype=jnp.float32) / HEAD)
    places = (start + jnp.arange(length, dtype=jnp.int32)).astype(jnp.float32)
    angles = places[:, None, None] * inverse[None, None, :]
    cosine_table = jnp.cos(angles)
    sine_table = jnp.sin(angles)
    pieces = block.astype(jnp.float32).reshape(length, -1, HEAD)
    leading = pieces[..., :middle]
    trailing = pieces[..., middle:]
    turned = jnp.concatenate(
        [
            leading * cosine_table - trailing * sine_table,
            trailing * cosine_table + leading * sine_table,
        ],
        -1,
    )
    return turned.reshape(length, -1).astype(jnp.bfloat16)


def window_attend(queries, keys, values, sink):
    rows_here = queries.shape[0]
    start = lax.axis_index("sp") * rows_here
    length = lax.axis_size("sp") * rows_here
    blocks = rows_here // WINDOW
    kv_width = keys.shape[1]
    kv_count = kv_width // HEAD
    head_count = queries.shape[1] // HEAD
    group = head_count // kv_count
    turned_q = rotary(queries, start)
    turned_k = rotary(keys, start)
    paired = jnp.concatenate([turned_k, values], 1)
    padded = padded_2(paired, (("sp", 0),), WINDOW)
    framed = padded.reshape(blocks + 2, WINDOW, 2 * kv_width)
    banded = jnp.concatenate([framed[:-2], framed[1:-1], framed[2:]], axis=1)
    key_band = banded[..., :kv_width].reshape(blocks, 3 * WINDOW, kv_count, HEAD)
    value_band = banded[..., kv_width:].reshape(blocks, 3 * WINDOW, kv_count, HEAD)
    query_blocks = turned_q.reshape(blocks, WINDOW, kv_count, group, HEAD)
    scores = jnp.einsum(
        "nqkgd,nskd->nkgqs", query_blocks, key_band, preferred_element_type=jnp.float32
    ) * HEAD ** (-0.5)
    query_place = (
        start + jnp.arange(blocks)[:, None, None] * WINDOW + jnp.arange(WINDOW)[None, :, None]
    )
    key_place = (
        start
        + jnp.arange(blocks)[:, None, None] * WINDOW
        - WINDOW
        + jnp.arange(3 * WINDOW)[None, None, :]
    )
    valid = (jnp.abs(key_place - query_place) <= WINDOW) & (key_place >= 0) & (key_place < length)
    scores = jnp.where(valid[:, None, None], scores, -jnp.inf)
    sink_grid = sink.reshape(kv_count, group)[None, :, :, None]
    top = jnp.maximum(jnp.max(scores, -1), sink_grid)
    raised = jnp.exp(scores - top[..., None])
    denom = jnp.sum(raised, -1) + jnp.exp(sink_grid - top)
    weights = (raised / denom[..., None]).astype(jnp.bfloat16)
    output = jnp.einsum(
        "nkgqs,nskd->nqkgd", weights, value_band, preferred_element_type=jnp.float32
    )
    return output.astype(jnp.bfloat16).reshape(rows_here, head_count * HEAD)


def collect_weights(gate_weight, up_weight, down_weight):
    return (
        lax.all_gather(gate_weight, "sp", axis=0, tiled=True),
        lax.all_gather(up_weight, "sp", axis=0, tiled=True),
        lax.all_gather(down_weight, "sp", axis=1, tiled=True),
    )


def local(
    queries, keys, values, sink, stream, out_weight, norm_gain, gate_weight, up_weight, down_weight
):
    attended = window_attend(queries, keys, values, sink)
    gathered = collect_weights(gate_weight, up_weight, down_weight)
    gate_whole, up_whole, down_whole = gathered
    rows = attended
    projected = lax.psum_scatter(
        jnp.dot(rows, out_weight, preferred_element_type=jnp.float32),
        "tp",
        scatter_dimension=0,
        tiled=True,
    )
    mixed = (stream.astype(jnp.float32) + projected).astype(jnp.bfloat16)
    mixed_wide = mixed.astype(jnp.float32)
    scale = lax.rsqrt(jnp.mean(mixed_wide * mixed_wide, -1, keepdims=True) + 1e-06)
    normed = (mixed_wide * scale * norm_gain).astype(jnp.bfloat16)
    piece = lax.all_gather(normed, "tp", axis=0, tiled=True)
    gate = jnp.dot(piece, gate_whole, preferred_element_type=jnp.float32)
    upward = jnp.dot(piece, up_whole, preferred_element_type=jnp.float32)
    hidden = (jax.nn.silu(gate) * upward).astype(jnp.bfloat16)
    rows = hidden
    lowered = lax.psum_scatter(
        jnp.dot(rows, down_whole, preferred_element_type=jnp.float32).astype(jnp.bfloat16),
        "tp",
        scatter_dimension=0,
        tiled=True,
    ).astype(jnp.float32)
    return (mixed_wide + 0.5 * lowered).astype(jnp.bfloat16)


def turned(block, start):
    length, width = block.shape
    middle = HEAD // 2
    inverse = 1.0 / 10000.0 ** (jnp.arange(0, HEAD, 2, dtype=F32) / HEAD)
    places = (start + jnp.arange(length, dtype=jnp.int32)).astype(F32)
    angles = places[:, None] * inverse[None, :]
    cosine, sine = jnp.cos(angles), jnp.sin(angles)
    heads = width // HEAD
    cosine = jnp.tile(jnp.concatenate([cosine, cosine], 1), (1, heads))
    sine = jnp.tile(jnp.concatenate([-sine, sine], 1), (1, heads))
    cells = block.astype(F32)
    ahead = jnp.roll(cells, -middle, 1)
    behind = jnp.roll(cells, middle, 1)
    lower = (jnp.arange(width) % HEAD < middle)[None]
    return (cells * cosine + jnp.where(lower, ahead, behind) * sine).astype(BF)


def layer_kernel(
    dims, q_ref, kv_ref, sink_ref, stream_ref, w_ref, gain_ref, gu_own, gu_send, d_own, d_send,
    out_ref,
    kv, att, near, far, p_send, p_recv, kept, y_send, y_recv, mixed, na, nb, gu, dn,
    hid, c_send, c_recv, acc, s1a, r1a, s1b, r1b, s2a, r2a, s2b, r2b,
    gu_rs, d_rs, z_ss, x_ss, h_ss, h_rs, p_ss, p_rs, n_ss, n_rs, e_ss, e_rs,
):
    length, tokens, rows, per, tail, total = dims
    s = lax.axis_index("sp")
    z, x = s // 2, s % 2
    t = lax.axis_index("tp")
    y, c = t // 2, t % 2
    across = s + 1 - 2 * x
    at_x = {"sp": across}
    at_y = {"tp": t + 2 - 4 * y}
    at_c = {"tp": t + 1 - 2 * c}
    has_up, has_down = z < length - 1, z > 0
    last = 2 * length - 1

    def send(src, dst, ssem, rsem, to):
        return pltpu.make_async_remote_copy(
            src_ref=src, dst_ref=dst, send_sem=ssem, recv_sem=rsem,
            device_id=to, device_id_type=MESH,
        )

    barrier = pltpu.get_barrier_semaphore()

    def greet(to):
        pl.semaphore_signal(barrier, inc=1, device_id=to, device_id_type=MESH)

    greet(at_x)
    greet(at_y)
    greet(at_c)
    pl.when(has_up)(lambda: greet({"sp": s + 2}))
    pl.when(has_down)(lambda: greet({"sp": s - 2}))
    hop_up = (x == 1) & has_up
    hop_down = (x == 0) & has_down
    pl.when(hop_up)(lambda: greet({"sp": s + 1}))
    pl.when(hop_down)(lambda: greet({"sp": s - 1}))
    count = 3 + has_up.astype(jnp.int32) + has_down.astype(jnp.int32)
    count = count + hop_up.astype(jnp.int32) + hop_down.astype(jnp.int32)
    pl.semaphore_wait(barrier, count)

    after = send(kv_ref.at[pl.ds(tokens - WINDOW, WINDOW)], kv.at[pl.ds(0, WINDOW)], h_ss.at[0], h_rs.at[0], {"sp": s + 1})
    before = send(kv_ref.at[pl.ds(0, WINDOW)], kv.at[pl.ds(tokens + WINDOW, WINDOW)], h_ss.at[1], h_rs.at[1], {"sp": s - 1})
    pl.when(s < last)(after.start)
    pl.when(s > 0)(before.start)

    x_gu = send(gu_send, gu.at[s], x_ss.at[0], gu_rs.at[s], at_x)
    x_d = send(d_send, dn.at[s], x_ss.at[1], d_rs.at[s], at_x)
    x_gu.start()

    def line(kind, src, slot, index, side, way):
        buf, sems = ((gu, gu_rs), (dn, d_rs))[kind]
        to = {"sp": s + 2} if way == 0 else {"sp": s - 2}
        return send(src, buf.at[slot], z_ss.at[kind, way, index, side], sems.at[slot], to)

    def at_index(index):
        if index == 0:
            return z
        tables = ((0, 1, 2, 3), (1, 0, 2, 3), (2, 3, 1, 0), (3, 2, 1, 0))
        place = jnp.int32(tables[length - 1][index])
        for k in range(length - 1):
            place = jnp.where(z == k, tables[k][index], place)
        return place

    def landed(kind, slot):
        buf, sems = ((gu, gu_rs), (dn, d_rs))[kind]
        send(buf.at[slot], buf.at[slot], x_ss.at[0], sems.at[slot], at_x).wait_recv()

    def ways(index):
        if index == 0:
            return (has_up, has_down)
        place = at_index(index)
        return ((place < z) & has_up, (place > z) & has_down)

    def slot_of(index, side):
        return 2 * at_index(index) + (x if side == 0 else 1 - x)

    def push(kind, index, side):
        slot = slot_of(index, side)
        own = index == 0 and side == 0
        buf = (gu, dn)[kind]
        if not own:
            landed(kind, slot)
        src = (gu_own, d_own)[kind] if own else buf.at[slot]
        for way, cond in enumerate(ways(index)):
            pl.when(cond)(line(kind, src, slot, index, side, way).start)

    push(0, 0, 0)
    x_d.start()
    kv[pl.ds(WINDOW, tokens), :] = kv_ref[...]
    gu[s] = gu_own[...]
    dn[s] = d_own[...]

    @pl.when(s == 0)
    def _():
        kv[pl.ds(0, WINDOW), :] = jnp.zeros((WINDOW, kv.shape[1]), BF)

    @pl.when(s == last)
    def _():
        kv[pl.ds(tokens + WINDOW, WINDOW), :] = jnp.zeros((WINDOW, kv.shape[1]), BF)

    pl.when(s > 0)(after.wait_recv)
    pl.when(s < last)(before.wait_recv)

    kv_width = kv.shape[1] // 2
    heads = q_ref.shape[1] // HEAD
    group = heads // (kv_width // HEAD)

    def attend(n, carry):
        base = pl.multiple_of(n * WINDOW, WINDOW)
        shape = (WINDOW, 3 * WINDOW)
        q_at = lax.broadcasted_iota(jnp.int32, shape, 0)
        k_at = lax.broadcasted_iota(jnp.int32, shape, 1) - WINDOW
        place = k_at + (s * tokens + base)
        valid = (jnp.abs(k_at - q_at) <= WINDOW) & (place >= 0) & (place < total)
        outs = []
        for h in range(heads):
            g = h // group
            q = q_ref[pl.ds(base, WINDOW), h * HEAD : (h + 1) * HEAD]
            k = kv[pl.ds(base, 3 * WINDOW), g * HEAD : (g + 1) * HEAD]
            v = kv[pl.ds(base, 3 * WINDOW), kv_width + g * HEAD : kv_width + (g + 1) * HEAD]
            sc = lax.dot_general(q, k, (((1,), (1,)), ((), ())), preferred_element_type=F32)
            sc = jnp.where(valid, sc * HEAD ** (-0.5), -jnp.inf)
            sink = sink_ref[h]
            top = jnp.maximum(jnp.max(sc, -1, keepdims=True), sink)
            raised = jnp.exp(sc - top)
            denom = jnp.sum(raised, -1, keepdims=True) + jnp.exp(sink - top)
            weights = (raised / denom).astype(BF)
            outs.append(jnp.dot(weights, v, preferred_element_type=F32).astype(BF))
            if h % 2:
                att[pl.ds(base, WINDOW), (h - 1) * HEAD : (h + 1) * HEAD] = jnp.concatenate(outs[-2:], 1)
        return carry

    blocks = tokens // WINDOW
    lax.fori_loop(0, blocks - 1, attend, 0)
    push(0, 0, 1)
    lax.fori_loop(blocks - 1, blocks, attend, 0)

    for dy in range(2):
        yy = y if dy == 0 else 1 - y
        mine = pl.multiple_of((2 * yy + c) * rows, 32)
        theirs = pl.multiple_of((2 * yy + 1 - c) * rows, 32)
        near[pl.ds(dy * rows, rows), :] = att[pl.ds(mine, rows), :]
        far[pl.ds(dy * rows, rows), :] = att[pl.ds(theirs, rows), :]
    model = out_ref.shape[1]
    step = 4 * LANES

    def project_far(n, carry):
        cols = pl.ds(pl.multiple_of(n * step, step), step)
        p_send[:, cols] = jnp.dot(far[...], w_ref[:, cols], preferred_element_type=F32).astype(BF)
        return carry

    def project_near(n, carry):
        cols = pl.ds(pl.multiple_of(n * step, step), step)
        kept[:, cols] = jnp.dot(near[...], w_ref[:, cols], preferred_element_type=F32)
        return carry

    lax.fori_loop(0, model // step, project_far, 0)
    by_core = send(p_send, p_recv, p_ss.at[0], p_rs.at[0], at_c)
    by_core.start()
    lax.fori_loop(0, model // step, project_near, 0)
    push(0, 1, 0)
    by_core.wait_recv()
    y_send[...] = (kept[rows:, :] + p_recv[rows:, :].astype(F32)).astype(BF)
    by_y = send(y_send, y_recv, p_ss.at[1], p_rs.at[1], at_y)
    by_y.start()
    by_y.wait_recv()
    mix = stream_ref[...].astype(F32) + (kept[:rows, :] + p_recv[:rows, :].astype(F32) + y_recv[...].astype(F32))
    mix = mix.astype(BF)
    mixed[...] = mix
    wide = mix.astype(F32)
    scale = lax.rsqrt(jnp.mean(wide * wide, -1, keepdims=True) + 1e-06)
    normed = (wide * scale * gain_ref[...]).astype(BF)
    cut = model // 2
    na[0, 0] = normed[:, :cut]
    nb[0, 0] = normed[:, cut:]

    a_x = send(na.at[0, 0], na.at[0, 1], n_ss.at[0], n_rs.at[0], at_x)
    b_y = send(nb.at[0, 0], nb.at[0, 2], n_ss.at[1], n_rs.at[1], at_y)
    a_y0 = send(na.at[0, 0], na.at[0, 2], n_ss.at[2], n_rs.at[2], at_y)
    a_y1 = send(na.at[0, 1], na.at[0, 3], n_ss.at[3], n_rs.at[3], at_y)
    b_x0 = send(nb.at[0, 0], nb.at[0, 1], n_ss.at[4], n_rs.at[4], at_x)
    b_x1 = send(nb.at[0, 2], nb.at[0, 3], n_ss.at[5], n_rs.at[5], at_x)
    a_x.start()
    b_y.start()
    a_y0.start()
    b_x0.start()
    push(0, 1, 1)
    a_x.wait_recv()
    a_y1.start()
    b_y.wait_recv()
    b_x1.start()
    push(0, 2, 0)
    a_y0.wait_recv()
    a_y1.wait_recv()
    b_x0.wait_recv()
    b_x1.wait_recv()
    a_c = send(na.at[0], na.at[1], n_ss.at[6], n_rs.at[6], at_c)
    b_c = send(nb.at[0], nb.at[1], n_ss.at[7], n_rs.at[7], at_c)
    a_c.start()
    b_c.start()
    push(0, 2, 1)
    push(1, 0, 0)
    push(1, 0, 1)
    for index in range(3, length):
        push(0, index, 0)
        push(0, index, 1)

    def units(q, cols, size):
        half = size // 2
        depth = gu.shape[1]
        lhs = na[q].reshape(4 * rows, cut)
        rhs = nb[q].reshape(4 * rows, cut)
        one = gu[pl.ds(0, length), :, cols].reshape(length * depth, size)
        two = gu[pl.ds(length, length), :, cols].reshape(length * depth, size)
        both = jnp.dot(lhs, one, preferred_element_type=F32) + jnp.dot(rhs, two, preferred_element_type=F32)
        gate = both[:, :half]
        return (gate / (1.0 + jnp.exp(-gate)) * both[:, half:]).astype(BF)

    def hidden_of(q):
        def body(n, carry):
            cols = pl.ds(pl.multiple_of(n * 2 * LANES, 2 * LANES), 2 * LANES)
            hid[q, :, pl.ds(pl.multiple_of(n * LANES, LANES), LANES)] = units(q, cols, 2 * LANES)
            return carry

        lax.fori_loop(0, per, body, 0)
        hid[q, :, per * LANES :] = units(q, pl.ds(per * 2 * LANES, 2 * tail), 2 * tail)

    hidden_of(0)
    a_c.wait_recv()
    b_c.wait_recv()
    push(1, 1, 0)
    push(1, 1, 1)
    hidden_of(1)

    part = d_own.shape[1]

    def exchange(k, which):
        src, dst, to = (
            (c_send.at[k], c_recv.at[k], at_c),
            (s1a.at[k], r1a.at[k], at_x),
            (s1b.at[k], r1b.at[k], at_y),
            (s2a.at[k], r2a.at[k], at_y),
            (s2b.at[k], r2b.at[k], at_x),
        )[which]
        return send(src, dst, e_ss.at[which, k], e_rs.at[which, k], to)

    def second(k):
        exchange(k, 1).wait_recv()
        exchange(k, 2).wait_recv()
        a = [acc[k, 0, 2 * dy] + r1a[k, dy].astype(F32) for dy in range(2)]
        b = [acc[k, 1, dx] + r1b[k, dx].astype(F32) for dx in range(2)]
        s2a[k] = a[1].astype(BF)
        s2b[k] = b[1].astype(BF)
        exchange(k, 3).start()
        exchange(k, 4).start()
        acc[k, 0, 0] = a[0]
        acc[k, 1, 0] = b[0]

    for k in range(length):
        if k > 1:
            push(1, k, 0)
            push(1, k, 1)
        low = 2 * at_index(k)
        for side in range(2):
            weight = dn[low + side]
            c_send[k, side] = jnp.dot(hid[1], weight, preferred_element_type=F32).astype(BF)
        exchange(k, 0).start()
        for side in range(2):
            weight = dn[low + side]
            acc[k, side] = jnp.dot(hid[0], weight, preferred_element_type=F32).reshape(4, rows, part)
        if k:
            second(k - 1)
        exchange(k, 0).wait_recv()
        acc[k] = acc[k] + c_recv[k].reshape(2, 4, rows, part).astype(F32)
        for dy in range(2):
            s1a[k, dy] = acc[k, 0, 2 * dy + 1].astype(BF)
        for dx in range(2):
            s1b[k, dx] = acc[k, 1, 2 + dx].astype(BF)
        exchange(k, 1).start()
        exchange(k, 2).start()
    second(length - 1)
    for k in range(length):
        exchange(k, 3).wait_recv()
        exchange(k, 4).wait_recv()
        for side, got in ((0, r2a), (1, r2b)):
            cols = pl.ds(pl.multiple_of((2 * at_index(k) + side) * part, part), part)
            lowered = acc[k, side, 0] + got[k].astype(F32)
            out_ref[:, cols] = (mixed[:, cols].astype(F32) + 0.5 * lowered).astype(BF)

    pl.when(s < last)(after.wait_send)
    pl.when(s > 0)(before.wait_send)
    for copy in (x_gu, x_d, by_core, by_y, a_x, b_y, a_y0, a_y1, b_x0, b_x1, a_c, b_c):
        copy.wait_send()
    for k in range(length):
        for which in range(5):
            exchange(k, which).wait_send()
    for kind in range(2):
        for index in range(length):
            for side in range(2):
                slot = slot_of(index, side)
                own = index == 0 and side == 0
                src = (gu_own, d_own)[kind] if own else (gu, dn)[kind].at[slot]
                for way, cond in enumerate(ways(index)):
                    pl.when(cond)(line(kind, src, slot, index, side, way).wait_send)


def local_lines(
    queries, keys, values, sink, stream, out_weight, norm_gain, gate_weight, up_weight, down_weight
):
    length = lax.axis_size("sp") // 2
    s = lax.axis_index("sp")
    tokens = queries.shape[0]
    rows, model = stream.shape
    depth, wide = gate_weight.shape
    per = wide // LANES // 2
    tail = wide // 2 - per * LANES
    half = wide // 2
    edge = 2 * per * LANES

    def pieces(x):
        out = []
        for n in range(per):
            at = (x * per + n) * LANES
            out += [gate_weight[:, at : at + LANES], up_weight[:, at : at + LANES]]
        at = edge + x * tail
        out += [gate_weight[:, at : at + tail], up_weight[:, at : at + tail]]
        return jnp.concatenate(out, 1)

    def lowers(x):
        at = x * per * LANES
        end = edge + x * tail
        return jnp.concatenate([down_weight[at : at + per * LANES], down_weight[end : end + tail]], 0)

    first = s % 2 == 0
    gu_0, gu_1, d_0, d_1 = pieces(0), pieces(1), lowers(0), lowers(1)
    paired = jnp.concatenate([turned(keys, s * tokens), values], 1)
    part = down_weight.shape[1]
    vmem = pl.BlockSpec(memory_space=pltpu.VMEM)
    dma = pltpu.SemaphoreType.DMA
    dims = (length, tokens, rows, per, tail, tokens * 2 * length)
    return pl.pallas_call(
        functools.partial(layer_kernel, dims),
        out_shape=jax.ShapeDtypeStruct((rows, model), BF),
        in_specs=[vmem, vmem, pl.BlockSpec(memory_space=pltpu.SMEM)] + [vmem] * 7,
        out_specs=vmem,
        scratch_shapes=[
            pltpu.VMEM((tokens + 2 * WINDOW, paired.shape[1]), BF),
            pltpu.VMEM(queries.shape, BF),
            pltpu.VMEM((2 * rows, queries.shape[1]), BF),
            pltpu.VMEM((2 * rows, queries.shape[1]), BF),
            pltpu.VMEM((2 * rows, model), BF),
            pltpu.VMEM((2 * rows, model), BF),
            pltpu.VMEM((2 * rows, model), F32),
            pltpu.VMEM((rows, model), BF),
            pltpu.VMEM((rows, model), BF),
            pltpu.VMEM((rows, model), BF),
            pltpu.VMEM((2, 4, rows, model // 2), BF),
            pltpu.VMEM((2, 4, rows, model // 2), BF),
            pltpu.VMEM((2 * length, depth, 2 * half), BF),
            pltpu.VMEM((2 * length, half, part), BF),
            pltpu.VMEM((2, 4 * rows, half), BF),
            pltpu.VMEM((length, 2, 4 * rows, part), BF),
            pltpu.VMEM((length, 2, 4 * rows, part), BF),
            pltpu.VMEM((length, 2, 4, rows, part), F32),
        ]
        + [pltpu.VMEM((length, 2, rows, part), BF)] * 4
        + [pltpu.VMEM((length, rows, part), BF)] * 4
        + [
            dma((2 * length,)), dma((2 * length,)), dma((2, 2, length, 2)), dma((2,)),
            dma((2,)), dma((2,)), dma((2,)), dma((2,)), dma((8,)), dma((8,)),
            dma((5, length)), dma((5, length)),
        ],
        compiler_params=pltpu.CompilerParams(
            collective_id=0, has_side_effects=True, vmem_limit_bytes=63 * 1024 * 1024
        ),
    )(
        turned(queries, s * tokens), paired, sink, stream, out_weight, norm_gain[None],
        jnp.where(first, gu_0, gu_1), jnp.where(first, gu_1, gu_0),
        jnp.where(first, d_0, d_1), jnp.where(first, d_1, d_0),
    )


def solution(mesh):
    placed = (
        P("sp", "tp"),
        P("sp", "tp"),
        P("sp", "tp"),
        P("tp"),
        P(("sp", "tp"), None),
        P("tp", None),
        P(),
        P("sp", "tp"),
        P("sp", "tp"),
        P("tp", "sp"),
    )
    lines = mesh.shape["tp"] == 4 and mesh.shape["sp"] == 8
    return jax.shard_map(
        local_lines if lines else local, mesh=mesh, in_specs=placed, out_specs=P(("sp", "tp"), None), check_vma=False
    )
```

```python
import functools

import jax
import jax.numpy as jnp
from jax import lax
from jax.experimental import pallas as pl
from jax.experimental.pallas import tpu as pltpu
from jax.sharding import PartitionSpec as P

HEAD = 64
WINDOW = 128
LANES = 128
BF = jnp.bfloat16
F32 = jnp.float32
MESH = pl.DeviceIdType.MESH


def padded_2(cells, sides, width):
    for axis, dim in sides:
        count = lax.axis_size(axis)
        ends = count - 1
        head = lax.slice_in_dim(cells, 0, width, axis=dim)
        tail = lax.slice_in_dim(cells, cells.shape[dim] - width, cells.shape[dim], axis=dim)
        cells = jnp.concatenate(
            [
                lax.ppermute(tail, axis, [(i, (i + 1) % count) for i in range(ends)]),
                cells,
                lax.ppermute(head, axis, [((i + 1) % count, i) for i in range(ends)]),
            ],
            axis=dim,
        )
    return cells


def rotary(block, start):
    length = block.shape[0]
    middle = HEAD // 2
    inverse = 1.0 / 10000.0 ** (jnp.arange(0, HEAD, 2, dtype=jnp.float32) / HEAD)
    places = (start + jnp.arange(length, dtype=jnp.int32)).astype(jnp.float32)
    angles = places[:, None, None] * inverse[None, None, :]
    cosine_table = jnp.cos(angles)
    sine_table = jnp.sin(angles)
    pieces = block.astype(jnp.float32).reshape(length, -1, HEAD)
    leading = pieces[..., :middle]
    trailing = pieces[..., middle:]
    turned = jnp.concatenate(
        [
            leading * cosine_table - trailing * sine_table,
            trailing * cosine_table + leading * sine_table,
        ],
        -1,
    )
    return turned.reshape(length, -1).astype(jnp.bfloat16)


def window_attend(queries, keys, values, sink):
    rows_here = queries.shape[0]
    start = lax.axis_index("sp") * rows_here
    length = lax.axis_size("sp") * rows_here
    blocks = rows_here // WINDOW
    kv_width = keys.shape[1]
    kv_count = kv_width // HEAD
    head_count = queries.shape[1] // HEAD
    group = head_count // kv_count
    turned_q = rotary(queries, start)
    turned_k = rotary(keys, start)
    paired = jnp.concatenate([turned_k, values], 1)
    padded = padded_2(paired, (("sp", 0),), WINDOW)
    framed = padded.reshape(blocks + 2, WINDOW, 2 * kv_width)
    banded = jnp.concatenate([framed[:-2], framed[1:-1], framed[2:]], axis=1)
    key_band = banded[..., :kv_width].reshape(blocks, 3 * WINDOW, kv_count, HEAD)
    value_band = banded[..., kv_width:].reshape(blocks, 3 * WINDOW, kv_count, HEAD)
    query_blocks = turned_q.reshape(blocks, WINDOW, kv_count, group, HEAD)
    scores = jnp.einsum(
        "nqkgd,nskd->nkgqs", query_blocks, key_band, preferred_element_type=jnp.float32
    ) * HEAD ** (-0.5)
    query_place = (
        start + jnp.arange(blocks)[:, None, None] * WINDOW + jnp.arange(WINDOW)[None, :, None]
    )
    key_place = (
        start
        + jnp.arange(blocks)[:, None, None] * WINDOW
        - WINDOW
        + jnp.arange(3 * WINDOW)[None, None, :]
    )
    valid = (jnp.abs(key_place - query_place) <= WINDOW) & (key_place >= 0) & (key_place < length)
    scores = jnp.where(valid[:, None, None], scores, -jnp.inf)
    sink_grid = sink.reshape(kv_count, group)[None, :, :, None]
    top = jnp.maximum(jnp.max(scores, -1), sink_grid)
    raised = jnp.exp(scores - top[..., None])
    denom = jnp.sum(raised, -1) + jnp.exp(sink_grid - top)
    weights = (raised / denom[..., None]).astype(jnp.bfloat16)
    output = jnp.einsum(
        "nkgqs,nskd->nqkgd", weights, value_band, preferred_element_type=jnp.float32
    )
    return output.astype(jnp.bfloat16).reshape(rows_here, head_count * HEAD)


def collect_weights(gate_weight, up_weight, down_weight):
    return (
        lax.all_gather(gate_weight, "sp", axis=0, tiled=True),
        lax.all_gather(up_weight, "sp", axis=0, tiled=True),
        lax.all_gather(down_weight, "sp", axis=1, tiled=True),
    )


def local(
    queries, keys, values, sink, stream, out_weight, norm_gain, gate_weight, up_weight, down_weight
):
    attended = window_attend(queries, keys, values, sink)
    gathered = collect_weights(gate_weight, up_weight, down_weight)
    gate_whole, up_whole, down_whole = gathered
    rows = attended
    projected = lax.psum_scatter(
        jnp.dot(rows, out_weight, preferred_element_type=jnp.float32),
        "tp",
        scatter_dimension=0,
        tiled=True,
    )
    mixed = (stream.astype(jnp.float32) + projected).astype(jnp.bfloat16)
    mixed_wide = mixed.astype(jnp.float32)
    scale = lax.rsqrt(jnp.mean(mixed_wide * mixed_wide, -1, keepdims=True) + 1e-06)
    normed = (mixed_wide * scale * norm_gain).astype(jnp.bfloat16)
    piece = lax.all_gather(normed, "tp", axis=0, tiled=True)
    gate = jnp.dot(piece, gate_whole, preferred_element_type=jnp.float32)
    upward = jnp.dot(piece, up_whole, preferred_element_type=jnp.float32)
    hidden = (jax.nn.silu(gate) * upward).astype(jnp.bfloat16)
    rows = hidden
    lowered = lax.psum_scatter(
        jnp.dot(rows, down_whole, preferred_element_type=jnp.float32).astype(jnp.bfloat16),
        "tp",
        scatter_dimension=0,
        tiled=True,
    ).astype(jnp.float32)
    return (mixed_wide + 0.5 * lowered).astype(jnp.bfloat16)


def turn_tables(length, start):
    lane = jnp.arange(LANES)
    pair = (lane % (HEAD // 2)).astype(F32) * 2.0
    inverse = 1.0 / 10000.0 ** (pair / HEAD)
    places = (start + jnp.arange(length, dtype=jnp.int32)).astype(F32)
    angles = places[:, None] * inverse[None, :]
    side = jnp.where(lane % HEAD < HEAD // 2, -1.0, 1.0).astype(F32)
    return jnp.cos(angles), jnp.sin(angles) * side[None, :]


def turned(block, cosine, sine):
    cells = block.astype(F32)
    lane = lax.broadcasted_iota(jnp.int32, cells.shape, 1)
    ahead = pltpu.roll(cells, LANES - HEAD // 2, 1)
    behind = pltpu.roll(cells, HEAD // 2, 1)
    other = jnp.where(lane % HEAD < HEAD // 2, ahead, behind)
    return (cells * cosine + other * sine).astype(BF)


def layer_kernel(
    dims, q_ref, kv_ref, cos_ref, sin_ref, sink_ref, stream_ref, w_ref, gain_ref, gu_own, gu_send, d_own, d_send,
    out_ref,
    kv, att, near, far, p_send, p_recv, kept, y_send, y_recv, mixed, na, nb, gu, dn,
    hid, c_send, c_recv, acc, s1a, r1a, s1b, r1b, s2a, r2a, s2b, r2b,
    gu_rs, d_rs, z_ss, x_ss, h_ss, h_rs, p_ss, p_rs, n_ss, n_rs, e_ss, e_rs,
):
    length, tokens, rows, per, tail, total = dims
    s = lax.axis_index("sp")
    z, x = s // 2, s % 2
    t = lax.axis_index("tp")
    y, c = t // 2, t % 2
    across = s + 1 - 2 * x
    at_x = {"sp": across}
    at_y = {"tp": t + 2 - 4 * y}
    at_c = {"tp": t + 1 - 2 * c}
    has_up, has_down = z < length - 1, z > 0
    last = 2 * length - 1

    def send(src, dst, ssem, rsem, to):
        return pltpu.make_async_remote_copy(
            src_ref=src, dst_ref=dst, send_sem=ssem, recv_sem=rsem,
            device_id=to, device_id_type=MESH,
        )

    barrier = pltpu.get_barrier_semaphore()

    def greet(to):
        pl.semaphore_signal(barrier, inc=1, device_id=to, device_id_type=MESH)

    greet(at_x)
    greet(at_y)
    greet(at_c)
    pl.when(has_up)(lambda: greet({"sp": s + 2}))
    pl.when(has_down)(lambda: greet({"sp": s - 2}))
    hop_up = (x == 1) & has_up
    hop_down = (x == 0) & has_down
    pl.when(hop_up)(lambda: greet({"sp": s + 1}))
    pl.when(hop_down)(lambda: greet({"sp": s - 1}))
    count = 3 + has_up.astype(jnp.int32) + has_down.astype(jnp.int32)
    count = count + hop_up.astype(jnp.int32) + hop_down.astype(jnp.int32)
    pl.semaphore_wait(barrier, count)

    after = send(kv_ref.at[pl.ds(tokens - WINDOW, WINDOW)], kv.at[pl.ds(0, WINDOW)], h_ss.at[0], h_rs.at[0], {"sp": s + 1})
    before = send(kv_ref.at[pl.ds(0, WINDOW)], kv.at[pl.ds(tokens + WINDOW, WINDOW)], h_ss.at[1], h_rs.at[1], {"sp": s - 1})
    pl.when(s < last)(after.start)
    pl.when(s > 0)(before.start)

    x_gu = send(gu_send, gu.at[s], x_ss.at[0], gu_rs.at[s], at_x)
    x_d = send(d_send, dn.at[s], x_ss.at[1], d_rs.at[s], at_x)
    x_gu.start()

    def line(kind, src, slot, index, side, way):
        buf, sems = ((gu, gu_rs), (dn, d_rs))[kind]
        to = {"sp": s + 2} if way == 0 else {"sp": s - 2}
        return send(src, buf.at[slot], z_ss.at[kind, way, index, side], sems.at[slot], to)

    def at_index(index):
        if index == 0:
            return z
        tables = ((0, 1, 2, 3), (1, 0, 2, 3), (2, 3, 1, 0), (3, 2, 1, 0))
        place = jnp.int32(tables[length - 1][index])
        for k in range(length - 1):
            place = jnp.where(z == k, tables[k][index], place)
        return place

    def landed(kind, slot):
        buf, sems = ((gu, gu_rs), (dn, d_rs))[kind]
        send(buf.at[slot], buf.at[slot], x_ss.at[0], sems.at[slot], at_x).wait_recv()

    def ways(index):
        if index == 0:
            return (has_up, has_down)
        place = at_index(index)
        return ((place < z) & has_up, (place > z) & has_down)

    def slot_of(index, side):
        return 2 * at_index(index) + (x if side == 0 else 1 - x)

    def push(kind, index, side):
        slot = slot_of(index, side)
        own = index == 0 and side == 0
        buf = (gu, dn)[kind]
        if not own:
            landed(kind, slot)
        src = (gu_own, d_own)[kind] if own else buf.at[slot]
        for way, cond in enumerate(ways(index)):
            pl.when(cond)(line(kind, src, slot, index, side, way).start)

    middle = has_up & has_down

    def relay(kind, index, side):
        pl.when(middle)(lambda: push(kind, index, side))

    def settle(kind, index, side):
        pl.when(jnp.logical_not(middle))(lambda: landed(kind, slot_of(index, side)))

    push(0, 0, 0)
    push(1, 0, 0)
    x_d.start()
    kv[pl.ds(WINDOW, tokens), :] = kv_ref[...]
    gu[s] = gu_own[...]
    dn[s] = d_own[...]

    @pl.when(s == 0)
    def _():
        kv[pl.ds(0, WINDOW), :] = jnp.zeros((WINDOW, kv.shape[1]), BF)

    @pl.when(s == last)
    def _():
        kv[pl.ds(tokens + WINDOW, WINDOW), :] = jnp.zeros((WINDOW, kv.shape[1]), BF)

    pl.when(s > 0)(after.wait_recv)
    pl.when(s < last)(before.wait_recv)

    kv_width = kv.shape[1] // 2
    heads = q_ref.shape[1] // HEAD

    def turn_keys(n, carry):
        at = pl.ds(pl.multiple_of(n * WINDOW, WINDOW), WINDOW)
        for p in range(kv_width // LANES):
            cols = slice(p * LANES, (p + 1) * LANES)
            kv[at, cols] = turned(kv[at, cols], cos_ref[at, :], sin_ref[at, :])
        return carry

    lax.fori_loop(0, tokens // WINDOW + 2, turn_keys, 0)
    group = heads // (kv_width // HEAD)

    def attend(n, carry):
        base = pl.multiple_of(n * WINDOW, WINDOW)
        shape = (WINDOW, 3 * WINDOW)
        q_at = lax.broadcasted_iota(jnp.int32, shape, 0)
        k_at = lax.broadcasted_iota(jnp.int32, shape, 1) - WINDOW
        place = k_at + (s * tokens + base)
        valid = (jnp.abs(k_at - q_at) <= WINDOW) & (place >= 0) & (place < total)
        outs = []
        for h in range(heads):
            g = h // group
            if h % 2 == 0:
                here = pl.ds(pl.multiple_of(base + WINDOW, WINDOW), WINDOW)
                two = q_ref[pl.ds(base, WINDOW), h * HEAD : (h + 2) * HEAD]
                two = turned(two, cos_ref[here, :], sin_ref[here, :])
            q = two[:, HEAD * (h % 2) : HEAD * (h % 2 + 1)]
            k = kv[pl.ds(base, 3 * WINDOW), g * HEAD : (g + 1) * HEAD]
            v = kv[pl.ds(base, 3 * WINDOW), kv_width + g * HEAD : kv_width + (g + 1) * HEAD]
            sc = lax.dot_general(q, k, (((1,), (1,)), ((), ())), preferred_element_type=F32)
            sc = jnp.where(valid, sc * HEAD ** (-0.5), -jnp.inf)
            sink = sink_ref[h]
            top = jnp.maximum(jnp.max(sc, -1, keepdims=True), sink)
            raised = jnp.exp(sc - top)
            denom = jnp.sum(raised, -1, keepdims=True) + jnp.exp(sink - top)
            weights = (raised / denom).astype(BF)
            outs.append(jnp.dot(weights, v, preferred_element_type=F32).astype(BF))
            if h % 2:
                att[pl.ds(base, WINDOW), (h - 1) * HEAD : (h + 1) * HEAD] = jnp.concatenate(outs[-2:], 1)
        return carry

    blocks = tokens // WINDOW
    def between(n, carry):
        attend(n, carry)

        @pl.when(n == blocks - 3)
        def _():
            push(0, 0, 1)

        @pl.when(n == blocks - 2)
        def _():
            relay(0, 1, 0)
            relay(0, 2, 0)

        return carry

    lax.fori_loop(0, blocks, between, 0)
    push(1, 0, 1)

    for dy in range(2):
        yy = y if dy == 0 else 1 - y
        mine = pl.multiple_of((2 * yy + c) * rows, 32)
        theirs = pl.multiple_of((2 * yy + 1 - c) * rows, 32)
        near[pl.ds(dy * rows, rows), :] = att[pl.ds(mine, rows), :]
        far[pl.ds(dy * rows, rows), :] = att[pl.ds(theirs, rows), :]
    model = out_ref.shape[1]
    step = 4 * LANES

    def project_far(n, carry):
        cols = pl.ds(pl.multiple_of(n * step, step), step)
        p_send[:, cols] = jnp.dot(far[...], w_ref[:, cols], preferred_element_type=F32).astype(BF)
        return carry

    def project_near(n, carry):
        cols = pl.ds(pl.multiple_of(n * step, step), step)
        kept[:, cols] = jnp.dot(near[...], w_ref[:, cols], preferred_element_type=F32)
        return carry

    lax.fori_loop(0, model // step, project_far, 0)
    by_core = send(p_send, p_recv, p_ss.at[0], p_rs.at[0], at_c)
    by_core.start()
    lax.fori_loop(0, model // step, project_near, 0)
    by_core.wait_recv()
    y_send[...] = (kept[rows:, :] + p_recv[rows:, :].astype(F32)).astype(BF)
    by_y = send(y_send, y_recv, p_ss.at[1], p_rs.at[1], at_y)
    by_y.start()
    relay(0, 1, 1)
    relay(0, 2, 1)
    by_y.wait_recv()
    mix = stream_ref[...].astype(F32) + (kept[:rows, :] + p_recv[:rows, :].astype(F32) + y_recv[...].astype(F32))
    mix = mix.astype(BF)
    mixed[...] = mix
    wide = mix.astype(F32)
    scale = lax.rsqrt(jnp.mean(wide * wide, -1, keepdims=True) + 1e-06)
    normed = (wide * scale * gain_ref[...]).astype(BF)
    cut = model // 2
    na[0, 0] = normed[:, :cut]
    nb[0, 0] = normed[:, cut:]

    a_x = send(na.at[0, 0], na.at[0, 1], n_ss.at[0], n_rs.at[0], at_x)
    b_y = send(nb.at[0, 0], nb.at[0, 2], n_ss.at[1], n_rs.at[1], at_y)
    a_y0 = send(na.at[0, 0], na.at[0, 2], n_ss.at[2], n_rs.at[2], at_y)
    a_y1 = send(na.at[0, 1], na.at[0, 3], n_ss.at[3], n_rs.at[3], at_y)
    b_x0 = send(nb.at[0, 0], nb.at[0, 1], n_ss.at[4], n_rs.at[4], at_x)
    b_x1 = send(nb.at[0, 2], nb.at[0, 3], n_ss.at[5], n_rs.at[5], at_x)
    a_x.start()
    b_y.start()
    a_y0.start()
    b_x0.start()
    relay(0, 3, 0)
    a_x.wait_recv()
    a_y1.start()
    b_y.wait_recv()
    b_x1.start()
    a_y0.wait_recv()
    a_y1.wait_recv()
    b_x0.wait_recv()
    b_x1.wait_recv()
    a_c = send(na.at[0], na.at[1], n_ss.at[6], n_rs.at[6], at_c)
    b_c = send(nb.at[0], nb.at[1], n_ss.at[7], n_rs.at[7], at_c)
    a_c.start()
    b_c.start()
    relay(0, 3, 1)
    for index in (1, 2):
        for side in range(2):
            relay(1, index, side)
    for index in range(1, length):
        for side in range(2):
            settle(0, index, side)

    def units(q, cols, size):
        half = size // 2
        depth = gu.shape[1]
        lhs = na[q].reshape(4 * rows, cut)
        rhs = nb[q].reshape(4 * rows, cut)
        one = gu[pl.ds(0, length), :, cols].reshape(length * depth, size)
        two = gu[pl.ds(length, length), :, cols].reshape(length * depth, size)
        both = jnp.dot(lhs, one, preferred_element_type=F32) + jnp.dot(rhs, two, preferred_element_type=F32)
        gate = both[:, :half]
        return (gate / (1.0 + jnp.exp(-gate)) * both[:, half:]).astype(BF)

    def hidden_of(q):
        def body(n, carry):
            cols = pl.ds(pl.multiple_of(n * 2 * LANES, 2 * LANES), 2 * LANES)
            hid[q, :, pl.ds(pl.multiple_of(n * LANES, LANES), LANES)] = units(q, cols, 2 * LANES)
            return carry

        lax.fori_loop(0, per, body, 0)
        hid[q, :, per * LANES :] = units(q, pl.ds(per * 2 * LANES, 2 * tail), 2 * tail)

    hidden_of(0)
    relay(1, 3, 0)
    a_c.wait_recv()
    b_c.wait_recv()
    hidden_of(1)
    relay(1, 3, 1)

    part = d_own.shape[1]

    def exchange(k, which):
        src, dst, to = (
            (c_send.at[k], c_recv.at[k], at_c),
            (s1a.at[k], r1a.at[k], at_x),
            (s1b.at[k], r1b.at[k], at_y),
            (s2a.at[k], r2a.at[k], at_y),
            (s2b.at[k], r2b.at[k], at_x),
        )[which]
        return send(src, dst, e_ss.at[which, k], e_rs.at[which, k], to)

    def second(k):
        exchange(k, 1).wait_recv()
        exchange(k, 2).wait_recv()
        a = [acc[k, 0, 2 * dy] + r1a[k, dy].astype(F32) for dy in range(2)]
        b = [acc[k, 1, dx] + r1b[k, dx].astype(F32) for dx in range(2)]
        s2a[k] = a[1].astype(BF)
        s2b[k] = b[1].astype(BF)
        exchange(k, 3).start()
        exchange(k, 4).start()
        acc[k, 0, 0] = a[0]
        acc[k, 1, 0] = b[0]

    for k in range(length):
        if k:
            settle(1, k, 0)
            settle(1, k, 1)
        low = 2 * at_index(k)
        for side in range(2):
            weight = dn[low + side]
            c_send[k, side] = jnp.dot(hid[1], weight, preferred_element_type=F32).astype(BF)
        exchange(k, 0).start()
        for side in range(2):
            weight = dn[low + side]
            acc[k, side] = jnp.dot(hid[0], weight, preferred_element_type=F32).reshape(4, rows, part)
        if k:
            second(k - 1)
        exchange(k, 0).wait_recv()
        acc[k] = acc[k] + c_recv[k].reshape(2, 4, rows, part).astype(F32)
        for dy in range(2):
            s1a[k, dy] = acc[k, 0, 2 * dy + 1].astype(BF)
        for dx in range(2):
            s1b[k, dx] = acc[k, 1, 2 + dx].astype(BF)
        exchange(k, 1).start()
        exchange(k, 2).start()
    second(length - 1)
    for k in range(length):
        exchange(k, 3).wait_recv()
        exchange(k, 4).wait_recv()
        for side, got in ((0, r2a), (1, r2b)):
            cols = pl.ds(pl.multiple_of((2 * at_index(k) + side) * part, part), part)
            lowered = acc[k, side, 0] + got[k].astype(F32)
            out_ref[:, cols] = (mixed[:, cols].astype(F32) + 0.5 * lowered).astype(BF)

    pl.when(s < last)(after.wait_send)
    pl.when(s > 0)(before.wait_send)
    for copy in (x_gu, x_d, by_core, by_y, a_x, b_y, a_y0, a_y1, b_x0, b_x1, a_c, b_c):
        copy.wait_send()
    for k in range(length):
        for which in range(5):
            exchange(k, which).wait_send()
    for kind in range(2):
        for index in range(length):
            for side in range(2):
                slot = slot_of(index, side)
                own = index == 0 and side == 0
                src = (gu_own, d_own)[kind] if own else (gu, dn)[kind].at[slot]
                for way, cond in enumerate(ways(index)):
                    pl.when(cond)(line(kind, src, slot, index, side, way).wait_send)


def local_lines(
    queries, keys, values, sink, stream, out_weight, norm_gain, gate_weight, up_weight, down_weight
):
    length = lax.axis_size("sp") // 2
    s = lax.axis_index("sp")
    tokens = queries.shape[0]
    rows, model = stream.shape
    depth, wide = gate_weight.shape
    per = wide // LANES // 2
    tail = wide // 2 - per * LANES
    half = wide // 2
    edge = 2 * per * LANES

    def pieces(x):
        out = []
        for n in range(per):
            at = (x * per + n) * LANES
            out += [gate_weight[:, at : at + LANES], up_weight[:, at : at + LANES]]
        at = edge + x * tail
        out += [gate_weight[:, at : at + tail], up_weight[:, at : at + tail]]
        return jnp.concatenate(out, 1)

    def lowers(x):
        at = x * per * LANES
        end = edge + x * tail
        return jnp.concatenate([down_weight[at : at + per * LANES], down_weight[end : end + tail]], 0)

    first = s % 2 == 0
    gu_0, gu_1, d_0, d_1 = pieces(0), pieces(1), lowers(0), lowers(1)
    paired = jnp.concatenate([keys, values], 1)
    cosine, sine = turn_tables(tokens + 2 * WINDOW, s * tokens - WINDOW)
    part = down_weight.shape[1]
    vmem = pl.BlockSpec(memory_space=pltpu.VMEM)
    dma = pltpu.SemaphoreType.DMA
    dims = (length, tokens, rows, per, tail, tokens * 2 * length)
    return pl.pallas_call(
        functools.partial(layer_kernel, dims),
        out_shape=jax.ShapeDtypeStruct((rows, model), BF),
        in_specs=[vmem] * 4 + [pl.BlockSpec(memory_space=pltpu.SMEM)] + [vmem] * 7,
        out_specs=vmem,
        scratch_shapes=[
            pltpu.VMEM((tokens + 2 * WINDOW, paired.shape[1]), BF),
            pltpu.VMEM(queries.shape, BF),
            pltpu.VMEM((2 * rows, queries.shape[1]), BF),
            pltpu.VMEM((2 * rows, queries.shape[1]), BF),
            pltpu.VMEM((2 * rows, model), BF),
            pltpu.VMEM((2 * rows, model), BF),
            pltpu.VMEM((2 * rows, model), F32),
            pltpu.VMEM((rows, model), BF),
            pltpu.VMEM((rows, model), BF),
            pltpu.VMEM((rows, model), BF),
            pltpu.VMEM((2, 4, rows, model // 2), BF),
            pltpu.VMEM((2, 4, rows, model // 2), BF),
            pltpu.VMEM((2 * length, depth, 2 * half), BF),
            pltpu.VMEM((2 * length, half, part), BF),
            pltpu.VMEM((2, 4 * rows, half), BF),
            pltpu.VMEM((length, 2, 4 * rows, part), BF),
            pltpu.VMEM((length, 2, 4 * rows, part), BF),
            pltpu.VMEM((length, 2, 4, rows, part), F32),
        ]
        + [pltpu.VMEM((length, 2, rows, part), BF)] * 4
        + [pltpu.VMEM((length, rows, part), BF)] * 4
        + [
            dma((2 * length,)), dma((2 * length,)), dma((2, 2, length, 2)), dma((2,)),
            dma((2,)), dma((2,)), dma((2,)), dma((2,)), dma((8,)), dma((8,)),
            dma((5, length)), dma((5, length)),
        ],
        compiler_params=pltpu.CompilerParams(
            collective_id=0, has_side_effects=True, vmem_limit_bytes=63 * 1024 * 1024
        ),
    )(
        queries, paired, cosine, sine, sink, stream, out_weight, norm_gain[None],
        jnp.where(first, gu_0, gu_1), jnp.where(first, gu_1, gu_0),
        jnp.where(first, d_0, d_1), jnp.where(first, d_1, d_0),
    )


def solution(mesh):
    placed = (
        P("sp", "tp"),
        P("sp", "tp"),
        P("sp", "tp"),
        P("tp"),
        P(("sp", "tp"), None),
        P("tp", None),
        P(),
        P("sp", "tp"),
        P("sp", "tp"),
        P("tp", "sp"),
    )
    lines = mesh.shape["tp"] == 4 and mesh.shape["sp"] == 8
    return jax.shard_map(
        local_lines if lines else local, mesh=mesh, in_specs=placed, out_specs=P(("sp", "tp"), None), check_vma=False
    )
```
